32 devices in a mesh: grp: 2 (over y), ep: 4 (over z), tp: 4 (over x, core).
Axes of the slice: x: 2, y: 2, z: 4, core: 2. Of those that a mesh axis runs over, the one named last changes fastest.
Arguments:
- tokens: bfloat16 [48, 2048], P('grp', 'ep'), parts along dimension 0, may hold values from -70 to 70
- first_gain: float32 [2048], replicated, may hold values from 0.1 to 1.9
- w_query: bfloat16 [2048, 2048], P('ep', 'tp'), may hold values from -0.125 to 0.125
- w_key: bfloat16 [2048, 2048], P('ep', 'tp'), may hold values from -0.125 to 0.125
- w_value: bfloat16 [2048, 4096], P('ep', 'tp'), may hold values from -0.125 to 0.125
- w_outgate: bfloat16 [2048, 4096], P('ep', 'tp'), may hold values from -0.125 to 0.125
- w_input: bfloat16 [2048, 16], replicated, may hold values from -0.125 to 0.125
- w_forget: bfloat16 [2048, 16], replicated, may hold values from -0.125 to 0.125
- input_bias: float32 [16], replicated, may hold values from -3 to 3
- forget_bias: float32 [16], replicated, may hold values from -2 to 5
- head_gain: float32 [4096], replicated, may hold values from 0.1 to 1.9
- w_project: bfloat16 [4096, 2048], P('tp', 'ep'), may hold values from -0.09375 to 0.09375
- cell_state: float32 [48, 16, 128, 256], P(('grp', 'ep'), 'tp'), parts along dimension 0, may hold values from -6 to 6
- norm_state: float32 [48, 16, 128], P(('grp', 'ep'), 'tp'), parts along dimension 0, may hold values from -6 to 6
- max_state: float32 [48, 16], P(('grp', 'ep'), 'tp'), parts along dimension 0, may hold values from -110 to 110
- second_gain: float32 [2048], replicated, may hold values from 0.1 to 1.9
- routes: int32 [48, 2], P('grp'), parts along dimension 0, may hold values from 0 to 3, all different within a row; in each aligned block of 6 rows (0 to 5, 6 to 11, ...) at most 6 rows name the same one
- route_weight: float32 [48, 2], P('grp'), parts along dimension 0, may hold values from 0.2 to 1
- expert_gate: bfloat16 [4, 2048, 4096], P('ep', None, 'tp'), may hold values from -0.125 to 0.125
- expert_up: bfloat16 [4, 2048, 4096], P('ep', None, 'tp'), may hold values from -0.125 to 0.125
- expert_down: bfloat16 [4, 4096, 2048], P('ep', 'tp'), may hold values from -0.09375 to 0.09375
Outputs:
- layer_out: bfloat16 [48, 2048], P('grp', 'ep'), parts along dimension 0
- new_cell: float32 [48, 16, 128, 256], P(('grp', 'ep'), 'tp'), parts along dimension 0
- new_norm: float32 [48, 16, 128], P(('grp', 'ep'), 'tp'), parts along dimension 0
- new_max: float32 [48, 16], P(('grp', 'ep'), 'tp'), parts along dimension 0
The draws below stay inside these ranges and needn't reach their ends.
There are 2 independent parts, one for each index of `grp`. The reference program is written for one: setup_inputs(seed, part) draws one part's arguments, and reference() takes and returns one part's arrays. A program takes and returns all parts, laid end to end along the dimension named above; an argument that names none is the same for every part. Nothing has to cross between parts.
Inputs may be any that keep to these rules, and one draw needn't show every extreme that they name: `routes`: each sequence names 2 different experts. In each aligned block of 6 sequences no expert is named by more than 6 of them, a bound that some block reaches.
All inputs are finite; a program needn't handle non-finite values.
Results may differ from the reference program's by a relative error of at most 0.0065.
Values may be sent and summed in bfloat16 or wider, within the bound.
A program may use at most 64 MiB of HBM per device.

```python
import math
import jax
import jax.numpy as jnp
import numpy as np
from jax import lax

D = 2048
HEADS = 16
DK = 128
DV = 256
FF = 4096
TOP = 2
SEQ_DEV = 6
EXPERTS = 4
SEQS = 24
CAP = 6
N_EP = 4


def draw_tokens(key, part):
    key_base, key_cols = jax.random.split(key, 2)
    position = jnp.arange(D, dtype=jnp.float32) / D
    drawn = jnp.clip(jax.random.normal(key_base, (SEQS, D), jnp.float32), -4.0, 4.0)
    column_scale = 4.0 ** position * jax.random.uniform(key_cols, (D,), jnp.float32, 0.6, 1.2)
    values = drawn * column_scale
    return values.astype(jnp.bfloat16)


def draw_max_state(key, part):
    key_base = jax.random.fold_in(key, 0)
    drawn = jax.random.uniform(key_base, (SEQS, HEADS), jnp.float32, -3.0, 3.0)
    return drawn


def shard_levels(key, dims, shards, least, high):
    gain, own = 1.0, jax.random.fold_in(key, 6)
    for dim, blocks in shards:
        steps = jnp.exp(jax.random.uniform(jax.random.fold_in(own, dim), (blocks,), jnp.float32, least / len(shards), high / len(shards)))
        gain = gain * jnp.repeat(steps, dims[dim] // blocks).reshape([-1 if axis == dim else 1 for axis in range(len(dims))])
    return gain


def shared_out(own_key, own, number, rows, count, top, limit, skew):
    ranking = jax.random.permutation(own_key, count)
    crowded, ordinary = portions_of(count, rows * top, limit, skew, True), portions_of(count, rows * top, limit, skew, False)
    places = jnp.arange(count)

    def named(lengths, turn):
        used = int((lengths > 0).sum())
        fixed = max(1, used // 4)
        moved = fixed + (places - fixed + turn * (used - fixed)) % max(1, count - fixed)
        return jnp.zeros((count,), jnp.int32).at[ranking[jnp.where(places < fixed, places, moved)]].set(jnp.asarray(lengths, jnp.int32))

    lengths = jnp.where(number % 4 == 0, named(crowded, number // 4), named(ordinary, number - number // 4 - 1))
    mixed = jax.random.permutation(jax.random.fold_in(own, 3), count)
    donor, taker = mixed[0:count // 2 * 2:2], mixed[1:count // 2 * 2:2]
    margin = jnp.minimum(lengths[donor] - 1, limit - lengths[taker]) // 2
    margin = jnp.where((donor == ranking[0]) | (taker == ranking[0]) | (lengths[taker] == 0), 0, jnp.maximum(margin, 0))
    moved = jax.random.randint(jax.random.fold_in(own, 4), (count // 2,), 0, 1 << 20) % (margin + 1)
    lengths = lengths.at[donor].add(-moved).at[taker].add(moved)
    labels = jnp.searchsorted(jnp.cumsum(lengths), jnp.arange(rows * top), side="right").astype(jnp.int32)
    listing = labels.reshape(top, rows).T
    listing = listing[jax.random.permutation(jax.random.fold_in(own, 1), rows)]
    turn = jax.random.randint(jax.random.fold_in(own, 2), (rows, 1), 0, top)
    return jnp.take_along_axis(listing, (jnp.arange(top)[None, :] + turn) % top, axis=1)


def portions_of(number_of, total, limit, skew, full):
    loads = [(1 << 20) // math.isqrt(rank ** skew) + 1 for rank in range(1, number_of + 1)]
    largest = limit if full else min(limit, max(-(-total // number_of), total * loads[0] // sum(loads)))
    least = 1 if total - largest >= number_of - 1 else 0
    given, spare = [largest] + [least] * (number_of - 1), total - largest - least * (number_of - 1)
    while spare > 0:
        free = [i for i in range(1, number_of) if given[i] < largest] or [i for i in range(1, number_of) if given[i] < limit]
        whole, left = sum([loads[i] for i in free]), spare
        for i in free:
            extra = min(limit - given[i], max(1, left * loads[i] // whole), spare)
            given[i] = given[i] + extra
            spare = spare - extra
    return np.array(given)


def bell_draw(rng, shape, scale, reach, pieces=(), held_as=jnp.bfloat16):
    array = scale * jax.random.normal(rng, shape, jnp.float32)
    if pieces:
        array = array * shard_levels(rng, shape, pieces, -0.22, 0.18)
    return jnp.clip(array, -reach, reach).astype(held_as)


def setup_inputs(seed: int = 0, part: int = 0) -> dict:
    keys = jax.random.split(jax.random.key(seed), 22)
    part_splits = jax.random.split(jax.random.fold_in(keys[21], part), 22)
    tokens = draw_tokens(jax.random.fold_in(jax.random.fold_in(keys[21], part), 71), part)
    first_gain = jnp.clip(1.0 + 0.18 * jax.random.normal(keys[1], (D,), jnp.float32), 0.1, 1.9)
    w_query = bell_draw(keys[2], (D, HEADS * DK), D ** -0.5, 0.125, ((0, 4), (1, 4)))
    w_key = bell_draw(keys[3], (D, HEADS * DK), D ** -0.5, 0.125, ((0, 4), (1, 4)))
    w_value = bell_draw(keys[4], (D, HEADS * DV), D ** -0.5, 0.125, ((0, 4), (1, 4)))
    w_outgate = bell_draw(keys[5], (D, HEADS * DV), D ** -0.5, 0.125, ((0, 4), (1, 4)))
    w_input = bell_draw(keys[6], (D, HEADS), D ** -0.5, 0.125)
    w_forget = bell_draw(keys[7], (D, HEADS), D ** -0.5, 0.125)
    input_bias = jnp.clip(jax.random.uniform(keys[8], (HEADS,), jnp.float32, -3.0, 3.0), -3.0, 3.0)
    forget_bias = jnp.clip(jax.random.uniform(keys[9], (HEADS,), jnp.float32, -2.0, 5.0), -2.0, 5.0)
    head_gain = jnp.clip(1.0 + 0.18 * jax.random.normal(keys[10], (HEADS * DV,), jnp.float32), 0.1, 1.9)
    w_project = bell_draw(keys[11], (HEADS * DV, D), (HEADS * DV) ** -0.5, 0.09375, ((0, 4), (1, 4)))
    cell_state = bell_draw(part_splits[12], (SEQS, HEADS, DK, DV), 1.0, 6.0, ((0, 4), (1, 4)), jnp.float32)
    norm_state = bell_draw(part_splits[13], (SEQS, HEADS, DK), 1.0, 6.0, ((0, 4), (1, 4)), jnp.float32)
    max_state = draw_max_state(jax.random.fold_in(jax.random.fold_in(keys[21], part), 71), part)
    second_gain = jnp.clip(1.0 + 0.18 * jax.random.normal(keys[15], (D,), jnp.float32), 0.1, 1.9)
    routes_keys = jax.random.split(jax.random.fold_in(part_splits[16], 1), SEQS // SEQ_DEV)
    routes_turns = jax.random.permutation(jax.random.fold_in(part_splits[16], 3), SEQS // SEQ_DEV)
    routes = jax.vmap(lambda own, number: shared_out(jax.random.fold_in(part_splits[16], 2), own, number, SEQ_DEV, EXPERTS, TOP, CAP, 2))(routes_keys, routes_turns).reshape((SEQS, TOP))
    route_weight = jnp.clip(jnp.exp(jax.random.uniform(part_splits[17], (SEQS, TOP), jnp.float32, math.log(0.2), math.log(1.0))), 0.2, 1.0)
    expert_gate = bell_draw(keys[18], (EXPERTS, D, FF), D ** -0.5, 0.125, ((0, 4), (2, 4)))
    expert_up = bell_draw(keys[19], (EXPERTS, D, FF), D ** -0.5, 0.125, ((0, 4), (2, 4)))
    expert_down = bell_draw(keys[20], (EXPERTS, FF, D), FF ** -0.5, 0.09375, ((0, 4), (1, 4)))
    return dict(tokens=tokens, first_gain=first_gain, w_query=w_query, w_key=w_key, w_value=w_value, w_outgate=w_outgate, w_input=w_input, w_forget=w_forget, input_bias=input_bias, forget_bias=forget_bias, head_gain=head_gain, w_project=w_project, cell_state=cell_state, norm_state=norm_state, max_state=max_state, second_gain=second_gain, routes=routes, route_weight=route_weight, expert_gate=expert_gate, expert_up=expert_up, expert_down=expert_down)


NORM_EPS = 1e-05
HEAD_EPS = 1e-06

def layer_norm(stream_rows, gain_cols):
    values = stream_rows.astype(jnp.float32)
    row_mean = lax.optimization_barrier(jnp.mean(values, axis=1, keepdims=True))
    spread = lax.optimization_barrier(jnp.mean(values * values, axis=1, keepdims=True)) - row_mean * row_mean
    return ((values - row_mean) * lax.rsqrt(spread + NORM_EPS) * gain_cols).astype(jnp.bfloat16)

def routing_tables(routes, route_weight, blocks, capacity, experts):
    seq_total = routes.shape[0]
    seq_local = seq_total // blocks
    expert_ids = lax.broadcasted_iota(jnp.int32, (1, 1, experts), 2)
    matches = routes[:, :, None] == expert_ids
    routed = lax.optimization_barrier(jnp.sum(matches.astype(jnp.int32), axis=1))
    combine = lax.optimization_barrier(jnp.sum(jnp.where(matches, route_weight[:, :, None], 0.0), axis=1))
    running = jnp.cumsum(routed.reshape(blocks, seq_local, experts), axis=1).reshape(seq_total, experts) - routed
    block_ids = lax.broadcasted_iota(jnp.int32, (seq_total, experts), 0) // seq_local
    slot_of = block_ids * capacity + running
    slot_ids = lax.broadcasted_iota(jnp.int32, (experts, blocks * capacity, seq_total), 1)
    placed = (slot_of.T[:, None, :] == slot_ids) & (routed.T[:, None, :] > 0)
    return (placed, jnp.where(placed, combine.T[:, None, :], 0.0))

def reference(tokens, first_gain, w_query, w_key, w_value, w_outgate, w_input, w_forget, input_bias, forget_bias, head_gain, w_project, cell_state, norm_state, max_state, second_gain, routes, route_weight, expert_gate, expert_up, expert_down):
    normed = layer_norm(tokens, first_gain)
    queries = jnp.dot(normed, w_query, preferred_element_type=jnp.float32).astype(jnp.bfloat16)
    key_rows = jnp.dot(normed, w_key, preferred_element_type=jnp.float32).astype(jnp.bfloat16)
    value_rows = jnp.dot(normed, w_value, preferred_element_type=jnp.float32).astype(jnp.bfloat16)
    outgate = jnp.dot(normed, w_outgate, preferred_element_type=jnp.float32).astype(jnp.bfloat16)
    input_pre = jnp.dot(normed, w_input, preferred_element_type=jnp.float32) + input_bias
    forget_pre = jnp.dot(normed, w_forget, preferred_element_type=jnp.float32) + forget_bias
    carried = jax.nn.log_sigmoid(forget_pre) + max_state
    new_max = jnp.maximum(carried, input_pre)
    keep_old = jnp.exp(carried - new_max)
    admit_new = jnp.exp(input_pre - new_max)
    key_float = key_rows.astype(jnp.float32).reshape(SEQS, HEADS, DK)
    value_float = value_rows.astype(jnp.float32).reshape(SEQS, HEADS, DV)
    new_cell = keep_old[:, :, None, None] * cell_state + admit_new[:, :, None, None] * key_float[:, :, :, None] * value_float[:, :, None, :]
    new_norm = keep_old[:, :, None] * norm_state + admit_new[:, :, None] * key_float
    query_float = queries.astype(jnp.float32).reshape(SEQS, HEADS, DK) * DK ** (-0.5)
    readout = jnp.einsum('shk,shkv->shv', query_float, new_cell, precision=lax.Precision.HIGHEST)
    head_mean = lax.optimization_barrier(jnp.mean(readout, axis=2, keepdims=True))
    centred = readout - head_mean
    head_var = lax.optimization_barrier(jnp.mean(centred * centred, axis=2, keepdims=True))
    mixed_heads = ((centred * lax.rsqrt(head_var + HEAD_EPS)).reshape(SEQS, HEADS * DV) * head_gain * jax.nn.sigmoid(outgate.astype(jnp.float32))).astype(jnp.bfloat16)
    mixer_out = jnp.dot(mixed_heads, w_project, preferred_element_type=jnp.float32)
    stream = (tokens.astype(jnp.float32) + mixer_out).astype(jnp.bfloat16)
    second_normed = layer_norm(stream, second_gain)
    placed, weighted = routing_tables(routes, route_weight, N_EP, CAP, EXPERTS)
    picker = placed.astype(jnp.bfloat16)

    def one_expert(running_sum, packed):
        pick_rows, weight_rows, gate_w, up_w, down_w = packed
        chosen = jnp.dot(pick_rows, second_normed, preferred_element_type=jnp.float32).astype(jnp.bfloat16)
        gate_sum = jnp.dot(chosen, gate_w, preferred_element_type=jnp.float32)
        up_sum = jnp.dot(chosen, up_w, preferred_element_type=jnp.float32)
        active = (jax.nn.silu(gate_sum) * up_sum).astype(jnp.bfloat16)
        result = jnp.dot(active, down_w, preferred_element_type=jnp.float32).astype(jnp.bfloat16)
        added = jnp.dot(weight_rows.T, result.astype(jnp.float32), precision=lax.Precision.HIGHEST)
        return (running_sum + added, None)
    moe_out, unused = lax.scan(one_expert, jnp.zeros((SEQS, D), jnp.float32), (picker, weighted, expert_gate, expert_up, expert_down))
    layer_out = (stream.astype(jnp.float32) + moe_out).astype(jnp.bfloat16)
    return (layer_out, new_cell, new_norm, new_max)
```

```python
import functools

import jax
import jax.numpy as jnp
from jax import lax
from jax.experimental import pallas as pl
from jax.experimental.pallas import tpu as pltpu
from jax.sharding import PartitionSpec as P

NORM_EPS = 1e-05
HEAD_EPS = 1e-06
F32 = jnp.float32
BF16 = jnp.bfloat16
MESH = pl.DeviceIdType.MESH


def each(start, stop, body):
    if stop - start <= 16:
        for index in range(start, stop):
            body(index)
    else:
        lax.fori_loop(start, stop, lambda index, none: (body(index), none)[1], 0)


def tiles(width, body, most=256):
    size = min(width, most)
    if width == size:
        body(0, size)
    else:
        def step(index, none):
            body(pl.multiple_of(index * size, size), size)
            return none

        lax.fori_loop(0, width // size, step, 0)


def layer_kernel(
    E, T, SB, PB,
    tokens, first_gain, w_input, w_forget, input_bias, forget_bias, head_gain,
    norm_state, max_state, second_gain, routes, route_weight,
    w_query, w_key, w_value, w_outgate, w_project, cell_state, gate_w, up_w, down_w,
    layer_out, new_norm, new_max, key_out, value_out, keep_out,
    wall, wproj, cell, gate, up, down,
    tok_all, tok_pad, normed, pre_gate, proj_send, proj_recv, rows_out,
    mix_rows, mix_all, mix_mat, term_send, term_recv, stream_all, second, act,
    exp_send, exp_recv, final_send, final_recv, weight_rows, out_rows,
    load_sem, s0, r0, s1, r1, s2, r2, s3, r3, s4, r4, s5, r5, s6, r6,
):
    e = lax.axis_index("ep")
    t = lax.axis_index("tp")
    G = E * T
    S, C = tokens.shape
    SP = E * PB
    Hl, DK = norm_state.shape[1], norm_state.shape[2]
    DV = cell_state.shape[3]
    QW, VW = Hl * DK, Hl * DV

    loads = []
    starts = (
        (w_query, wall.at[:, 0:QW]),
        (w_key, wall.at[:, QW : 2 * QW]),
        (w_value, wall.at[:, 2 * QW : 2 * QW + VW]),
        (w_outgate, wall.at[:, 2 * QW + VW : 2 * QW + 2 * VW]),
        (cell_state, cell),
        (w_project, wproj),
        (gate_w.at[0], gate),
        (up_w.at[0], up),
        (down_w.at[0], down),
    )
    for number, (source, target) in enumerate(starts):
        loads.append(pltpu.make_async_copy(source, target, load_sem.at[number]))
        loads[-1].start()

    barrier = pltpu.get_barrier_semaphore()

    def peer(d):
        return lax.rem(e + d // T, E), lax.rem(t + d % T, T)

    def behind(d):
        return lax.rem(e + E - d // T, E), lax.rem(t + T - d % T, T)

    def greet(d):
        pe, pt = peer(d)
        pl.semaphore_signal(barrier, inc=1, device_id={"ep": pe, "tp": pt}, device_id_type=MESH)

    each(1, G, greet)
    pl.semaphore_wait(barrier, G - 1)

    def ep_copy(d, source, target, ss, rs):
        return pltpu.make_async_remote_copy(
            src_ref=source, dst_ref=target, send_sem=ss.at[d], recv_sem=rs.at[d],
            device_id={"ep": lax.rem(e + d, E)}, device_id_type=MESH,
        )

    def tp_copy(d, source, target, ss, rs):
        return pltpu.make_async_remote_copy(
            src_ref=source, dst_ref=target, send_sem=ss.at[d], recv_sem=rs.at[d],
            device_id={"tp": lax.rem(t + d, T)}, device_id_type=MESH,
        )

    def all_copy(d, source, target, ss, rs):
        pe, pt = peer(d)
        return pltpu.make_async_remote_copy(
            src_ref=source, dst_ref=target, send_sem=ss.at[d], recv_sem=rs.at[d],
            device_id={"ep": pe, "tp": pt}, device_id_type=MESH,
        )

    each(1, E, lambda d: ep_copy(d, tokens, tok_all.at[e], s0, r0).start())
    tok_all[e] = tokens[...]

    row = lax.broadcasted_iota(jnp.int32, (SP, S), 0)
    col = lax.broadcasted_iota(jnp.int32, (SP, S), 1)
    spread_f = jnp.where(((row // PB) * SB + row % PB == col) & (row % PB < SB), 1.0, 0.0).astype(F32)
    spread = spread_f.astype(BF16)
    weight = jnp.sum(jnp.where(routes[...] == e, route_weight[...], 0.0), axis=1, keepdims=True)
    weight = jnp.broadcast_to(weight, (S, 128))
    weight_rows[...] = jnp.dot(
        spread_f, weight, precision=lax.Precision.HIGHEST, preferred_element_type=F32
    ).reshape(E, PB, 128)

    each(1, E, lambda d: ep_copy(d, tokens, tok_all.at[lax.rem(e + E - d, E)], s0, r0).wait_recv())
    total = jnp.zeros((SP, 1), F32)
    square = jnp.zeros((SP, 1), F32)
    for b in range(E):
        x = jnp.dot(spread, tok_all[b], preferred_element_type=F32)
        tok_pad[b] = x
        total = total + jnp.sum(x, axis=1, keepdims=True)
        square = square + jnp.sum(x * x, axis=1, keepdims=True)
    mean = total / (E * C)
    inv = lax.rsqrt(square / (E * C) - mean * mean + NORM_EPS)
    for b in range(E):
        normed[b] = ((tok_pad[b] - mean) * inv * first_gain[b : b + 1, :]).astype(BF16)

    for load in loads[:4]:
        load.wait()

    mine = normed[e]

    def project(at, size):
        part = jnp.dot(mine, wall[:, pl.ds(at, size)], preferred_element_type=F32)
        proj_send[:, :, pl.ds(at, size)] = part.reshape(E, PB, size)

    tiles(wall.shape[1], project)

    def send_proj(d):
        ep_copy(d, proj_send.at[lax.rem(e + d, E)], proj_recv.at[e], s1, r1).start()

    each(1, E, send_proj)
    proj_recv[e] = proj_send[e]

    pre_i = jnp.zeros((SP, w_input.shape[1]), F32)
    pre_f = jnp.zeros((SP, w_input.shape[1]), F32)
    for b in range(E):
        pre_i = pre_i + jnp.dot(normed[b], w_input[b * C : (b + 1) * C, :], preferred_element_type=F32)
        pre_f = pre_f + jnp.dot(normed[b], w_forget[b * C : (b + 1) * C, :], preferred_element_type=F32)
    pre_gate[0] = (pre_i + input_bias[...]).reshape(E, PB, w_input.shape[1])
    pre_gate[1] = (pre_f + forget_bias[...]).reshape(E, PB, w_input.shape[1])
    my_i = pre_gate[0, e][:SB]
    my_f = pre_gate[1, e][:SB]
    lane = lax.broadcasted_iota(jnp.int32, my_i.shape, 1)
    keeps, admits = [], []
    for h in range(Hl):
        i_col = jnp.sum(jnp.where(lane == t * Hl + h, my_i, 0.0), axis=1, keepdims=True)
        f_col = jnp.sum(jnp.where(lane == t * Hl + h, my_f, 0.0), axis=1, keepdims=True)
        log_sig = jnp.minimum(f_col, 0.0) - jnp.log1p(jnp.exp(-jnp.abs(f_col)))
        carried = log_sig + max_state[:, h : h + 1]
        top = jnp.maximum(carried, i_col)
        keep = jnp.exp(carried - top)
        new_max[:, h : h + 1] = top
        keep_out[:, h : h + 1] = keep
        keeps.append(keep)
        admits.append(jnp.exp(i_col - top))
    mix_rows[...] = jnp.zeros_like(mix_rows)
    loads[4].wait()

    each(1, E, lambda d: ep_copy(d, proj_send.at[0], proj_recv.at[lax.rem(e + E - d, E)], s1, r1).wait_recv())
    summed = proj_recv[0]
    for b in range(1, E):
        summed = summed + proj_recv[b]
    rounded = summed.astype(BF16).astype(F32)
    gains = head_gain[pl.ds(t, 1), :]
    for h in range(Hl):
        q8 = rounded[:, h * DK : (h + 1) * DK] * (DK ** -0.5)
        k = rounded[:SB, QW + h * DK : QW + (h + 1) * DK]
        v = rounded[:SB, 2 * QW + h * DV : 2 * QW + (h + 1) * DV]
        gate_o = rounded[:SB, 2 * QW + VW + h * DV : 2 * QW + VW + (h + 1) * DV]
        turned = q8.T
        for s in range(SB):
            rows_out[s : s + 1, :] = jnp.sum(
                turned[:, s : s + 1] * cell[s, h], axis=0, keepdims=True
            )
        q_k = jnp.sum(q8[:SB] * k, axis=1, keepdims=True)
        read = keeps[h] * rows_out[0:SB, :] + (admits[h] * q_k) * v
        centred = read - jnp.mean(read, axis=1, keepdims=True)
        var = jnp.mean(centred * centred, axis=1, keepdims=True)
        mix_rows[0:SB, h * DV : (h + 1) * DV] = (
            centred * lax.rsqrt(var + HEAD_EPS) * gains[:, h * DV : (h + 1) * DV]
            * jax.nn.sigmoid(gate_o)
        )
        admitted = admits[h] * k
        key_out[:, h, :] = admitted
        value_out[:, h, :] = v
        new_norm[:, h, :] = keeps[h] * norm_state[:, h, :] + admitted
    mix_all[e] = mix_rows[...].astype(BF16)

    each(1, E, lambda d: ep_copy(d, mix_all.at[e], mix_all.at[e], s2, r2).start())
    loads[5].wait()
    each(1, E, lambda d: ep_copy(d, mix_all.at[e], mix_all.at[lax.rem(e + E - d, E)], s2, r2).wait_recv())
    mix_mat[...] = mix_all[...].astype(F32).reshape(SP, VW).astype(BF16)

    def out_project(at, size):
        part = jnp.dot(mix_mat[...], wproj[:, pl.ds(at, size)], preferred_element_type=F32)
        term_send[:, :, pl.ds(at, size)] = part.reshape(T, PB, size)

    tiles(C, out_project)
    each(1, T, lambda d: tp_copy(d, term_send.at[lax.rem(t + d, T)], term_recv.at[t], s3, r3).start())
    term_recv[t] = term_send[t]
    out_rows[...] = tok_pad[e].reshape(E, PB, C)
    each(1, T, lambda d: tp_copy(d, term_send.at[0], term_recv.at[lax.rem(t + T - d, T)], s3, r3).wait_recv())
    mixer = term_recv[0]
    for b in range(1, T):
        mixer = mixer + term_recv[b]
    stream_all[e, t] = (out_rows[t] + mixer).astype(BF16)

    each(1, G, lambda d: all_copy(d, stream_all.at[e, t], stream_all.at[e, t], s4, r4).start())

    def take_stream(d):
        be, bt = behind(d)
        all_copy(d, stream_all.at[e, t], stream_all.at[be, bt], s4, r4).wait_recv()

    for load in loads[6:8]:
        load.wait()
    each(1, G, take_stream)
    total = jnp.zeros((SP, 1), F32)
    square = jnp.zeros((SP, 1), F32)
    for b in range(E):
        x = stream_all[b].astype(F32).reshape(SP, C)
        tok_pad[b] = x
        total = total + jnp.sum(x, axis=1, keepdims=True)
        square = square + jnp.sum(x * x, axis=1, keepdims=True)
    mean = total / (E * C)
    inv = lax.rsqrt(square / (E * C) - mean * mean + NORM_EPS)
    for b in range(E):
        second[:, b * C : (b + 1) * C] = (
            (tok_pad[b] - mean) * inv * second_gain[b : b + 1, :]
        ).astype(BF16)

    def hidden(at, size):
        g = jnp.dot(second[...], gate[:, pl.ds(at, size)], preferred_element_type=F32)
        u = jnp.dot(second[...], up[:, pl.ds(at, size)], preferred_element_type=F32)
        act[:, pl.ds(at, size)] = (g * jax.nn.sigmoid(g) * u).astype(BF16)

    tiles(gate.shape[1], hidden)
    loads[8].wait()

    def lower(at, size):
        part = jnp.dot(act[...], down[:, pl.ds(at, size)], preferred_element_type=F32)
        exp_send[:, :, pl.ds(at, size)] = part.reshape(T, PB, size).astype(BF16)

    tiles(down.shape[1], lower)
    each(1, T, lambda d: tp_copy(d, exp_send.at[lax.rem(t + d, T)], exp_recv.at[t], s5, r5).start())
    exp_recv[t] = exp_send[t]
    each(1, T, lambda d: tp_copy(d, exp_send.at[0], exp_recv.at[lax.rem(t + T - d, T)], s5, r5).wait_recv())
    whole = exp_recv[0].astype(F32)
    for b in range(1, T):
        whole = whole + exp_recv[b].astype(F32)
    weighted = whole.astype(BF16).astype(F32) * weight_rows[t][:, 0:1]
    for b in range(E):
        final_send[b] = weighted[:, b * C : (b + 1) * C].astype(BF16)

    def send_final(d):
        pe, pt = peer(d)
        all_copy(d, final_send.at[pe], final_recv.at[e, t], s6, r6).start()

    each(1, G, send_final)
    final_recv[e, t] = final_send[e]

    def take_final(d):
        be, bt = behind(d)
        all_copy(d, final_send.at[0], final_recv.at[be, bt], s6, r6).wait_recv()

    each(1, G, take_final)
    moe = final_recv[0].astype(F32)
    for b in range(1, E):
        moe = moe + final_recv[b].astype(F32)
    done = (tok_pad[e] + moe.reshape(SP, C)).astype(BF16)
    back_row = lax.broadcasted_iota(jnp.int32, (S, SP), 0)
    back_col = lax.broadcasted_iota(jnp.int32, (S, SP), 1)
    gather = jnp.where((back_row // SB) * PB + back_row % SB == back_col, 1.0, 0.0).astype(BF16)
    layer_out[...] = jnp.dot(gather, done, preferred_element_type=F32).astype(BF16)

    each(1, E, lambda d: ep_copy(d, tokens, tok_all.at[e], s0, r0).wait_send())
    each(1, E, lambda d: ep_copy(d, proj_send.at[0], proj_recv.at[e], s1, r1).wait_send())
    each(1, E, lambda d: ep_copy(d, mix_all.at[e], mix_all.at[e], s2, r2).wait_send())
    each(1, T, lambda d: tp_copy(d, term_send.at[0], term_recv.at[t], s3, r3).wait_send())
    each(1, G, lambda d: all_copy(d, stream_all.at[e, t], stream_all.at[e, t], s4, r4).wait_send())
    each(1, T, lambda d: tp_copy(d, exp_send.at[0], exp_recv.at[t], s5, r5).wait_send())
    each(1, G, lambda d: all_copy(d, final_send.at[0], final_recv.at[e, t], s6, r6).wait_send())


def on_device(
    E, T,
    tokens, first_gain, w_query, w_key, w_value, w_outgate, w_input, w_forget,
    input_bias, forget_bias, head_gain, w_project, cell_state, norm_state, max_state,
    second_gain, routes, route_weight, expert_gate, expert_up, expert_down,
):
    S, C = tokens.shape
    SB, Hl, DK, DV = cell_state.shape
    D = first_gain.shape[0]
    FL = expert_gate.shape[2]
    PB = -(-SB // 8) * 8
    SP = E * PB
    heads = w_input.shape[1]
    width = 2 * Hl * (DK + DV)
    VW = Hl * DV
    vmem = pl.BlockSpec(memory_space=pltpu.VMEM)
    hbm = pl.BlockSpec(memory_space=pl.ANY)
    V = pltpu.VMEM
    dma = pltpu.SemaphoreType.DMA
    G = E * T
    layer_out, new_norm, new_max, admitted, values, keep = pl.pallas_call(
        functools.partial(layer_kernel, E, T, SB, PB),
        out_shape=(
            jax.ShapeDtypeStruct((S, C), BF16),
            jax.ShapeDtypeStruct((SB, Hl, DK), F32),
            jax.ShapeDtypeStruct((SB, Hl), F32),
            jax.ShapeDtypeStruct((SB, Hl, DK), F32),
            jax.ShapeDtypeStruct((SB, Hl, DV), F32),
            jax.ShapeDtypeStruct((SB, Hl), F32),
        ),
        in_specs=[vmem] * 12 + [hbm] * 9,
        out_specs=(vmem,) * 6,
        scratch_shapes=[
            V((C, width), BF16),
            V(w_project.shape, BF16),
            V(cell_state.shape, F32),
            V((D, FL), BF16),
            V((D, FL), BF16),
            V((FL, D), BF16),
            V((E, S, C), BF16),
            V((E, SP, C), F32),
            V((E, SP, C), BF16),
            V((2, E, PB, heads), F32),
            V((E, PB, width), F32),
            V((E, PB, width), F32),
            V((PB, DV), F32),
            V((PB, VW), F32),
            V((E, PB, VW), BF16),
            V((SP, VW), BF16),
            V((T, PB, C), F32),
            V((T, PB, C), F32),
            V((E, T, PB, C), BF16),
            V((SP, D), BF16),
            V((SP, FL), BF16),
            V((T, PB, D), BF16),
            V((T, PB, D), BF16),
            V((E, PB, C), BF16),
            V((E, T, PB, C), BF16),
            V((E, PB, 128), F32),
            V((E, PB, C), F32),
            dma((9,)),
            dma((E,)), dma((E,)), dma((E,)), dma((E,)), dma((E,)), dma((E,)),
            dma((T,)), dma((T,)), dma((G,)), dma((G,)), dma((T,)), dma((T,)),
            dma((G,)), dma((G,)),
        ],
        compiler_params=pltpu.CompilerParams(
            collective_id=0, has_side_effects=True, vmem_limit_bytes=56 * 1024 * 1024
        ),
        name="layer",
    )(
        tokens, first_gain.reshape(E, C), w_input, w_forget,
        input_bias.reshape(1, heads), forget_bias.reshape(1, heads),
        head_gain.reshape(T, VW), norm_state, max_state, second_gain.reshape(E, C),
        routes, route_weight,
        w_query, w_key, w_value, w_outgate, w_project, cell_state,
        expert_gate, expert_up, expert_down,
    )
    new_cell = (
        keep[:, :, None, None] * cell_state + admitted[:, :, :, None] * values[:, :, None, :]
    )
    return layer_out, new_cell, new_norm, new_max


def solution(mesh):
    placed = (
        P("grp", "ep"), P(), P("ep", "tp"), P("ep", "tp"), P("ep", "tp"), P("ep", "tp"),
        P(), P(), P(), P(), P(), P("tp", "ep"),
        P(("grp", "ep"), "tp", None, None), P(("grp", "ep"), "tp", None), P(("grp", "ep"), "tp"),
        P(), P("grp", None), P("grp", None),
        P("ep", None, "tp"), P("ep", None, "tp"), P("ep", "tp", None),
    )
    return jax.shard_map(
        functools.partial(on_device, mesh.shape["ep"], mesh.shape["tp"]),
        mesh=mesh,
        in_specs=placed,
        out_specs=(
            P("grp", "ep"),
            P(("grp", "ep"), "tp", None, None),
            P(("grp", "ep"), "tp", None),
            P(("grp", "ep"), "tp"),
        ),
        check_vma=False,
    )
```

```python
import functools

import jax
import jax.numpy as jnp
from jax import lax
from jax.experimental import pallas as pl
from jax.experimental.pallas import tpu as pltpu
from jax.sharding import PartitionSpec as P

NORM_EPS = 1e-05
HEAD_EPS = 1e-06
F32 = jnp.float32
BF16 = jnp.bfloat16
MESH = pl.DeviceIdType.MESH


def each(start, stop, body):
    if stop - start <= 16:
        for index in range(start, stop):
            body(index)
    else:
        lax.fori_loop(start, stop, lambda index, none: (body(index), none)[1], 0)


def tiles(width, body, most=256):
    size = next(s for s in (most, most // 2, width) if width % s == 0)
    if width == size:
        body(0, size)
    else:
        def step(index, none):
            body(pl.multiple_of(index * size, size), size)
            return none

        lax.fori_loop(0, width // size, step, 0)


def layer_kernel(
    E, T, SB, PB,
    tokens, first_gain, w_input, w_forget, input_bias, forget_bias, head_gain,
    norm_state, max_state, second_gain, routes, route_weight,
    w_query, w_key, w_value, w_outgate, w_project, cell_state, gate_w, up_w, down_w,
    layer_out, new_norm, new_max, key_out, value_out, keep_out,
    wall, wproj, cell, gate, up, down,
    tok_all, tok_pad, normed, pre_gate, proj_own, proj_send, proj_recv, rows_out,
    mix_rows, mix_all, mix_mat, term_send, term_recv, stream_all, second, act,
    exp_send, exp_recv, final_send, final_recv, weight_rows, out_rows,
    load_sem, s0, r0, s1, r1, s2, r2, s3, r3, s4, r4, s5, r5, s6, r6,
):
    e = lax.axis_index("ep")
    t = lax.axis_index("tp")
    G = E * T
    S, C = tokens.shape
    SP = E * PB
    Hl, DK = norm_state.shape[1], norm_state.shape[2]
    DV = cell_state.shape[3]
    QW, VW = Hl * DK, Hl * DV

    loads = []
    starts = (
        (w_query, wall.at[:, 0:QW]),
        (w_key, wall.at[:, QW : 2 * QW]),
        (w_value, wall.at[:, 2 * QW : 2 * QW + VW]),
        (w_outgate, wall.at[:, 2 * QW + VW : 2 * QW + 2 * VW]),
        (cell_state, cell),
        (w_project, wproj),
        (gate_w.at[0], gate),
        (up_w.at[0], up),
        (down_w.at[0], down),
    )
    for number, (source, target) in enumerate(starts):
        loads.append(pltpu.make_async_copy(source, target, load_sem.at[number]))
        loads[-1].start()

    for landing in (term_recv, mix_all, stream_all, exp_recv, final_recv):
        landing[...] = jnp.zeros_like(landing)

    barrier = pltpu.get_barrier_semaphore()

    def peer(d):
        return lax.rem(e + d // T, E), lax.rem(t + d % T, T)

    def behind(d):
        return lax.rem(e + E - d // T, E), lax.rem(t + T - d % T, T)

    def greet(d):
        pe, pt = peer(d)
        pl.semaphore_signal(barrier, inc=1, device_id={"ep": pe, "tp": pt}, device_id_type=MESH)

    each(1, G, greet)
    pl.semaphore_wait(barrier, G - 1)

    def ep_copy(d, source, target, ss, rs):
        return pltpu.make_async_remote_copy(
            src_ref=source, dst_ref=target, send_sem=ss.at[d], recv_sem=rs.at[d],
            device_id={"ep": lax.rem(e + d, E)}, device_id_type=MESH,
        )

    def tp_copy(d, source, target, ss, rs):
        return pltpu.make_async_remote_copy(
            src_ref=source, dst_ref=target, send_sem=ss.at[d], recv_sem=rs.at[d],
            device_id={"tp": lax.rem(t + d, T)}, device_id_type=MESH,
        )

    def all_copy(d, source, target, ss, rs):
        pe, pt = peer(d)
        return pltpu.make_async_remote_copy(
            src_ref=source, dst_ref=target, send_sem=ss.at[d], recv_sem=rs.at[d],
            device_id={"ep": pe, "tp": pt}, device_id_type=MESH,
        )

    each(1, E, lambda d: ep_copy(d, tokens, tok_all.at[e], s0, r0).start())
    tok_all[e] = tokens[...]

    row = lax.broadcasted_iota(jnp.int32, (SP, S), 0)
    col = lax.broadcasted_iota(jnp.int32, (SP, S), 1)
    spread_f = jnp.where(((row // PB) * SB + row % PB == col) & (row % PB < SB), 1.0, 0.0).astype(F32)
    spread = spread_f.astype(BF16)
    weight = jnp.sum(jnp.where(routes[...] == e, route_weight[...], 0.0), axis=0, keepdims=True)
    weight_rows[...] = jnp.broadcast_to(
        jnp.sum(jnp.where(spread_f > 0.0, weight, 0.0), axis=1, keepdims=True), (SP, 128)
    ).reshape(E, PB, 128)

    each(1, E, lambda d: ep_copy(d, tokens, tok_all.at[lax.rem(e + E - d, E)], s0, r0).wait_recv())
    total = jnp.zeros((SP, 1), F32)
    square = jnp.zeros((SP, 1), F32)
    for b in range(E):
        x = jnp.dot(spread, tok_all[b], preferred_element_type=F32)
        tok_pad[b] = x
        total = total + jnp.sum(x, axis=1, keepdims=True)
        square = square + jnp.sum(x * x, axis=1, keepdims=True)
    mean = total / (E * C)
    inv = lax.rsqrt(square / (E * C) - mean * mean + NORM_EPS)
    for b in range(E):
        normed[b] = ((tok_pad[b] - mean) * inv * first_gain[b * C : (b + 1) * C].reshape(1, C)).astype(BF16)

    for load in loads[:4]:
        load.wait()

    mine = normed[e]

    half = wall.shape[1] // 2

    def proj_copy(d, part, source, slot):
        cols = slice(part * half, (part + 1) * half)
        return ep_copy(
            d, proj_send.at[source, 0:SB, cols], proj_recv.at[slot, 0:SB, cols],
            s1.at[part], r1.at[part],
        )

    for part in range(2):

        def project(at, size, base=part * half):
            at = pl.multiple_of(base + at, size)
            total = jnp.dot(mine, wall[:, pl.ds(at, size)], preferred_element_type=F32)
            total = total.reshape(E, PB, size)
            proj_own[:, :, pl.ds(at, size)] = total
            proj_send[:, :, pl.ds(at, size)] = total.astype(BF16)

        tiles(half, project)
        each(1, E, lambda d: proj_copy(d, part, lax.rem(e + d, E), e).start())

    heads = w_input.shape[0]
    pre_i = jnp.zeros((SP, heads), F32)
    pre_f = jnp.zeros((SP, heads), F32)
    across = (((1,), (1,)), ((), ()))
    for b in range(E):
        cols = slice(b * C, (b + 1) * C)
        pre_i = pre_i + lax.dot_general(normed[b], w_input[:, cols], across, preferred_element_type=F32)
        pre_f = pre_f + lax.dot_general(normed[b], w_forget[:, cols], across, preferred_element_type=F32)
    pre_gate[0] = (pre_i + input_bias[...]).reshape(E, PB, heads)
    pre_gate[1] = (pre_f + forget_bias[...]).reshape(E, PB, heads)
    my_i = pre_gate[0, e][:SB]
    my_f = pre_gate[1, e][:SB]
    lane = lax.broadcasted_iota(jnp.int32, my_i.shape, 1)
    diag = lax.broadcasted_iota(jnp.int32, (SB, SB), 0) == lax.broadcasted_iota(jnp.int32, (SB, SB), 1)
    keeps, admits = [], []
    for h in range(Hl):
        i_col = jnp.sum(jnp.where(lane == t * Hl + h, my_i, 0.0), axis=1, keepdims=True)
        f_col = jnp.sum(jnp.where(lane == t * Hl + h, my_f, 0.0), axis=1, keepdims=True)
        log_sig = jnp.minimum(f_col, 0.0) - jnp.log1p(jnp.exp(-jnp.abs(f_col)))
        carried = log_sig + jnp.sum(jnp.where(diag, max_state[h : h + 1, :], 0.0), axis=1, keepdims=True)
        top = jnp.maximum(carried, i_col)
        keep = jnp.exp(carried - top)
        new_max[h : h + 1, :] = jnp.sum(jnp.where(diag, top, 0.0), axis=0, keepdims=True)
        keep_out[:, h : h + 1] = keep
        keeps.append(keep)
        admits.append(jnp.exp(i_col - top))
    mix_rows[...] = jnp.zeros_like(mix_rows)
    loads[4].wait()

    for part in range(2):
        each(1, E, lambda d: proj_copy(d, part, 0, lax.rem(e + E - d, E)).wait_recv())
    summed = proj_own[e]
    for d in range(1, E):
        summed = summed + proj_recv[lax.rem(e + E - d, E)].astype(F32)
    rounded = summed.astype(BF16).astype(F32)
    gains = head_gain[pl.ds(pl.multiple_of(t * VW, VW), VW)].reshape(1, VW)
    for h in range(Hl):
        q8 = rounded[:, h * DK : (h + 1) * DK] * (DK ** -0.5)
        k = rounded[:SB, QW + h * DK : QW + (h + 1) * DK]
        v = rounded[:SB, 2 * QW + h * DV : 2 * QW + (h + 1) * DV]
        gate_o = rounded[:SB, 2 * QW + VW + h * DV : 2 * QW + VW + (h + 1) * DV]
        turned = q8.T
        for s in range(SB):
            rows_out[s : s + 1, :] = jnp.sum(
                turned[:, s : s + 1] * cell[s, h], axis=0, keepdims=True
            )
        q_k = jnp.sum(q8[:SB] * k, axis=1, keepdims=True)
        read = keeps[h] * rows_out[0:SB, :] + (admits[h] * q_k) * v
        centred = read - jnp.mean(read, axis=1, keepdims=True)
        var = jnp.mean(centred * centred, axis=1, keepdims=True)
        mix_rows[0:SB, h * DV : (h + 1) * DV] = (
            centred * lax.rsqrt(var + HEAD_EPS) * gains[:, h * DV : (h + 1) * DV]
            * jax.nn.sigmoid(gate_o)
        )
        admitted = admits[h] * k
        key_out[:, h, :] = admitted
        value_out[:, h, :] = v
        new_norm[:, h, :] = keeps[h] * norm_state[:, h, :] + admitted
    mix_all[e] = mix_rows[...].astype(BF16)

    each(1, E, lambda d: ep_copy(d, mix_all.at[e, 0:SB], mix_all.at[e, 0:SB], s2, r2).start())
    loads[5].wait()
    each(1, E, lambda d: ep_copy(d, mix_all.at[e, 0:SB], mix_all.at[lax.rem(e + E - d, E), 0:SB], s2, r2).wait_recv())
    mix_mat[...] = mix_all[...].astype(F32).reshape(SP, VW).astype(BF16)

    def out_project(at, size):
        part = jnp.dot(mix_mat[...], wproj[:, pl.ds(at, size)], preferred_element_type=F32)
        term_send[:, :, pl.ds(at, size)] = part.reshape(T, PB, size)

    tiles(C, out_project)
    each(1, T, lambda d: tp_copy(d, term_send.at[lax.rem(t + d, T), 0:SB], term_recv.at[t, 0:SB], s3, r3).start())
    term_recv[t] = term_send[t]
    out_rows[...] = tok_pad[e].reshape(E, PB, C)
    each(1, T, lambda d: tp_copy(d, term_send.at[0, 0:SB], term_recv.at[lax.rem(t + T - d, T), 0:SB], s3, r3).wait_recv())
    mixer = term_recv[0]
    for b in range(1, T):
        mixer = mixer + term_recv[b]
    stream_all[e, t] = (out_rows[t] + mixer).astype(BF16)

    each(1, G, lambda d: all_copy(d, stream_all.at[e, t, 0:SB], stream_all.at[e, t, 0:SB], s4, r4).start())

    def take_stream(d):
        be, bt = behind(d)
        all_copy(d, stream_all.at[e, t, 0:SB], stream_all.at[be, bt, 0:SB], s4, r4).wait_recv()

    for load in loads[6:8]:
        load.wait()
    each(1, G, take_stream)
    total = jnp.zeros((SP, 1), F32)
    square = jnp.zeros((SP, 1), F32)
    for b in range(E):
        x = stream_all[b].astype(F32).reshape(SP, C)
        tok_pad[b] = x
        total = total + jnp.sum(x, axis=1, keepdims=True)
        square = square + jnp.sum(x * x, axis=1, keepdims=True)
    mean = total / (E * C)
    inv = lax.rsqrt(square / (E * C) - mean * mean + NORM_EPS)
    for b in range(E):
        second[:, b * C : (b + 1) * C] = (
            (tok_pad[b] - mean) * inv * second_gain[b * C : (b + 1) * C].reshape(1, C)
        ).astype(BF16)

    def hidden(at, size):
        g = jnp.dot(second[...], gate[:, pl.ds(at, size)], preferred_element_type=F32)
        u = jnp.dot(second[...], up[:, pl.ds(at, size)], preferred_element_type=F32)
        act[:, pl.ds(at, size)] = (g * jax.nn.sigmoid(g) * u).astype(BF16)

    tiles(gate.shape[1], hidden)
    loads[8].wait()

    mid = down.shape[1] // 2

    def exp_copy(d, part, source, slot):
        cols = slice(part * mid, (part + 1) * mid)
        return tp_copy(
            d, exp_send.at[source, 0:SB, cols], exp_recv.at[slot, 0:SB, cols],
            s5.at[part], r5.at[part],
        )

    for part in range(2):

        def lower(at, size, base=part * mid):
            at = pl.multiple_of(base + at, size)
            total = jnp.dot(act[...], down[:, pl.ds(at, size)], preferred_element_type=F32)
            exp_send[:, :, pl.ds(at, size)] = total.reshape(T, PB, size).astype(BF16)

        tiles(mid, lower)
        each(1, T, lambda d: exp_copy(d, part, lax.rem(t + d, T), t).start())
    exp_recv[t] = exp_send[t]
    for part in range(2):
        each(1, T, lambda d: exp_copy(d, part, 0, lax.rem(t + T - d, T)).wait_recv())
    whole = exp_recv[0].astype(F32)
    for b in range(1, T):
        whole = whole + exp_recv[b].astype(F32)
    weighted = whole.astype(BF16).astype(F32) * weight_rows[t][:, 0:1]
    for b in range(E):
        final_send[b] = weighted[:, b * C : (b + 1) * C].astype(BF16)

    def send_final(d):
        pe, pt = peer(d)
        all_copy(d, final_send.at[pe, 0:SB], final_recv.at[e, t, 0:SB], s6, r6).start()

    each(1, G, send_final)
    final_recv[e, t] = final_send[e]

    def take_final(d):
        be, bt = behind(d)
        all_copy(d, final_send.at[0, 0:SB], final_recv.at[be, bt, 0:SB], s6, r6).wait_recv()

    each(1, G, take_final)
    moe = final_recv[0].astype(F32)
    for b in range(1, E):
        moe = moe + final_recv[b].astype(F32)
    done = (tok_pad[e] + moe.reshape(SP, C)).astype(BF16)
    back_row = lax.broadcasted_iota(jnp.int32, (S, SP), 0)
    back_col = lax.broadcasted_iota(jnp.int32, (S, SP), 1)
    gather = jnp.where((back_row // SB) * PB + back_row % SB == back_col, 1.0, 0.0).astype(BF16)
    layer_out[...] = jnp.dot(gather, done, preferred_element_type=F32).astype(BF16)

    each(1, E, lambda d: ep_copy(d, tokens, tok_all.at[e], s0, r0).wait_send())
    for part in range(2):
        each(1, E, lambda d: proj_copy(d, part, 0, e).wait_send())
    each(1, E, lambda d: ep_copy(d, mix_all.at[e, 0:SB], mix_all.at[e, 0:SB], s2, r2).wait_send())
    each(1, T, lambda d: tp_copy(d, term_send.at[0, 0:SB], term_recv.at[t, 0:SB], s3, r3).wait_send())
    each(1, G, lambda d: all_copy(d, stream_all.at[e, t, 0:SB], stream_all.at[e, t, 0:SB], s4, r4).wait_send())
    for part in range(2):
        each(1, T, lambda d: exp_copy(d, part, 0, t).wait_send())
    each(1, G, lambda d: all_copy(d, final_send.at[0, 0:SB], final_recv.at[e, t, 0:SB], s6, r6).wait_send())


def on_device(
    E, T,
    tokens, first_gain, w_query, w_key, w_value, w_outgate, w_input, w_forget,
    input_bias, forget_bias, head_gain, w_project, cell_state, norm_state, max_state,
    second_gain, routes, route_weight, expert_gate, expert_up, expert_down,
):
    S, C = tokens.shape
    SB, Hl, DK, DV = cell_state.shape
    D = first_gain.shape[0]
    FL = expert_gate.shape[2]
    PB = -(-SB // 8) * 8
    SP = E * PB
    heads = w_input.shape[1]
    width = 2 * Hl * (DK + DV)
    VW = Hl * DV
    vmem = pl.BlockSpec(memory_space=pltpu.VMEM)
    hbm = pl.BlockSpec(memory_space=pl.ANY)
    V = pltpu.VMEM
    dma = pltpu.SemaphoreType.DMA
    G = E * T
    layer_out, new_norm, new_max, admitted, values, keep = pl.pallas_call(
        functools.partial(layer_kernel, E, T, SB, PB),
        out_shape=(
            jax.ShapeDtypeStruct((S, C), BF16),
            jax.ShapeDtypeStruct((SB, Hl, DK), F32),
            jax.ShapeDtypeStruct((Hl, SB), F32),
            jax.ShapeDtypeStruct((SB, Hl, DK), F32),
            jax.ShapeDtypeStruct((SB, Hl, DV), F32),
            jax.ShapeDtypeStruct((SB, Hl), F32),
        ),
        in_specs=[vmem] * 12 + [hbm] * 9,
        out_specs=(vmem,) * 6,
        scratch_shapes=[
            V((C, width), BF16),
            V(w_project.shape, BF16),
            V(cell_state.shape, F32),
            V((D, FL), BF16),
            V((D, FL), BF16),
            V((FL, D), BF16),
            V((E, S, C), BF16),
            V((E, SP, C), F32),
            V((E, SP, C), BF16),
            V((2, E, PB, heads), F32),
            V((E, PB, width), F32),
            V((E, PB, width), BF16),
            V((E, PB, width), BF16),
            V((PB, DV), F32),
            V((PB, VW), F32),
            V((E, PB, VW), BF16),
            V((SP, VW), BF16),
            V((T, PB, C), F32),
            V((T, PB, C), F32),
            V((E, T, PB, C), BF16),
            V((SP, D), BF16),
            V((SP, FL), BF16),
            V((T, PB, D), BF16),
            V((T, PB, D), BF16),
            V((E, PB, C), BF16),
            V((E, T, PB, C), BF16),
            V((E, PB, 128), F32),
            V((E, PB, C), F32),
            dma((9,)),
            dma((E,)), dma((E,)), dma((2, E)), dma((2, E)), dma((E,)), dma((E,)),
            dma((T,)), dma((T,)), dma((G,)), dma((G,)), dma((2, T)), dma((2, T)),
            dma((G,)), dma((G,)),
        ],
        compiler_params=pltpu.CompilerParams(
            collective_id=0, has_side_effects=True, vmem_limit_bytes=56 * 1024 * 1024
        ),
        name="layer",
    )(
        tokens, first_gain, w_input.T, w_forget.T,
        input_bias.reshape(1, heads), forget_bias.reshape(1, heads),
        head_gain, norm_state, max_state.T, second_gain,
        routes.T, route_weight.T,
        w_query, w_key, w_value, w_outgate, w_project, cell_state,
        expert_gate, expert_up, expert_down,
    )
    new_cell = (
        keep[:, :, None, None] * cell_state + admitted[:, :, :, None] * values[:, :, None, :]
    )
    return layer_out, new_cell, new_norm, new_max.T


def solution(mesh):
    placed = (
        P("grp", "ep"), P(), P("ep", "tp"), P("ep", "tp"), P("ep", "tp"), P("ep", "tp"),
        P(), P(), P(), P(), P(), P("tp", "ep"),
        P(("grp", "ep"), "tp", None, None), P(("grp", "ep"), "tp", None), P(("grp", "ep"), "tp"),
        P(), P("grp", None), P("grp", None),
        P("ep", None, "tp"), P("ep", None, "tp"), P("ep", "tp", None),
    )
    return jax.shard_map(
        functools.partial(on_device, mesh.shape["ep"], mesh.shape["tp"]),
        mesh=mesh,
        in_specs=placed,
        out_specs=(
            P("grp", "ep"),
            P(("grp", "ep"), "tp", None, None),
            P(("grp", "ep"), "tp", None),
            P(("grp", "ep"), "tp"),
        ),
        check_vma=False,
    )
```

```python
import functools

import jax
import jax.numpy as jnp
from jax import lax
from jax.experimental import pallas as pl
from jax.experimental.pallas import tpu as pltpu
from jax.sharding import PartitionSpec as P

NORM_EPS = 1e-05
HEAD_EPS = 1e-06
F32 = jnp.float32
BF16 = jnp.bfloat16
MESH = pl.DeviceIdType.MESH


def each(start, stop, body):
    if stop - start <= 16:
        for index in range(start, stop):
            body(index)
    else:
        lax.fori_loop(start, stop, lambda index, none: (body(index), none)[1], 0)


def tiles(width, body, most=256):
    size = next(s for s in (most, most // 2, width) if width % s == 0)
    if width == size:
        body(0, size)
    else:
        def step(index, none):
            body(pl.multiple_of(index * size, size), size)
            return none

        lax.fori_loop(0, width // size, step, 0)


def layer_kernel(
    E, T, SB, PB,
    tokens, first_gain, w_input, w_forget, input_bias, forget_bias, head_gain,
    norm_state, max_state, second_gain, routes, route_weight,
    w_query, w_key, w_value, w_outgate, w_project, cell_state, gate_w, up_w, down_w,
    layer_out, new_norm, new_max, key_out, value_out, keep_out,
    wall, wproj, cell, gate, up, down,
    tok_all, tok_pad, normed, pre_gate, proj_own, proj_send, proj_recv, rows_out,
    mix_rows, mix_all, mix_mat, term_send, term_recv, stream_all, second, act,
    exp_send, exp_recv, final_send, final_recv, weight_rows, out_rows,
    load_sem, s0, r0, s1, r1, s2, r2, s3, r3, s4, r4, s5, r5, s6, r6,
):
    e = lax.axis_index("ep")
    t = lax.axis_index("tp")
    G = E * T
    S, C = tokens.shape
    SP = E * PB
    Hl, DK = norm_state.shape[1], norm_state.shape[2]
    DV = cell_state.shape[3]
    QW, VW = Hl * DK, Hl * DV

    loads = []
    starts = (
        (w_query, wall.at[:, 0:QW]),
        (w_key, wall.at[:, QW : 2 * QW]),
        (w_value, wall.at[:, 2 * QW : 2 * QW + VW]),
        (w_outgate, wall.at[:, 2 * QW + VW : 2 * QW + 2 * VW]),
        (cell_state, cell),
        (w_project, wproj),
        (gate_w.at[0], gate),
        (up_w.at[0], up),
        (down_w.at[0], down),
    )
    for number, (source, target) in enumerate(starts):
        loads.append(pltpu.make_async_copy(source, target, load_sem.at[number]))
        loads[-1].start()

    for landing in (term_recv, mix_all, stream_all, exp_recv, final_recv):
        landing[...] = jnp.zeros_like(landing)

    barrier = pltpu.get_barrier_semaphore()

    def peer(d):
        return lax.rem(e + d // T, E), lax.rem(t + d % T, T)

    def behind(d):
        return lax.rem(e + E - d // T, E), lax.rem(t + T - d % T, T)

    def greet(d):
        pe, pt = peer(d)
        pl.semaphore_signal(barrier, inc=1, device_id={"ep": pe, "tp": pt}, device_id_type=MESH)

    each(1, G, greet)
    pl.semaphore_wait(barrier, G - 1)

    def ep_copy(d, source, target, ss, rs):
        return pltpu.make_async_remote_copy(
            src_ref=source, dst_ref=target, send_sem=ss.at[d], recv_sem=rs.at[d],
            device_id={"ep": lax.rem(e + d, E)}, device_id_type=MESH,
        )

    def tp_copy(d, source, target, ss, rs):
        return pltpu.make_async_remote_copy(
            src_ref=source, dst_ref=target, send_sem=ss.at[d], recv_sem=rs.at[d],
            device_id={"tp": lax.rem(t + d, T)}, device_id_type=MESH,
        )

    def all_copy(d, source, target, ss, rs):
        pe, pt = peer(d)
        return pltpu.make_async_remote_copy(
            src_ref=source, dst_ref=target, send_sem=ss.at[d], recv_sem=rs.at[d],
            device_id={"ep": pe, "tp": pt}, device_id_type=MESH,
        )

    each(1, E, lambda d: ep_copy(d, tokens, tok_all.at[e], s0, r0).start())
    tok_all[e] = tokens[...]

    row = lax.broadcasted_iota(jnp.int32, (SP, S), 0)
    col = lax.broadcasted_iota(jnp.int32, (SP, S), 1)
    spread_f = jnp.where(((row // PB) * SB + row % PB == col) & (row % PB < SB), 1.0, 0.0).astype(F32)
    spread = spread_f.astype(BF16)
    weight = jnp.sum(jnp.where(routes[...] == e, route_weight[...], 0.0), axis=0, keepdims=True)
    weight_rows[...] = jnp.broadcast_to(
        jnp.sum(jnp.where(spread_f > 0.0, weight, 0.0), axis=1, keepdims=True), (SP, 128)
    ).reshape(E, PB, 128)

    each(1, E, lambda d: ep_copy(d, tokens, tok_all.at[lax.rem(e + E - d, E)], s0, r0).wait_recv())
    total = jnp.zeros((SP, 1), F32)
    square = jnp.zeros((SP, 1), F32)
    for b in range(E):
        x = jnp.dot(spread, tok_all[b], preferred_element_type=F32)
        tok_pad[b] = x
        total = total + jnp.sum(x, axis=1, keepdims=True)
        square = square + jnp.sum(x * x, axis=1, keepdims=True)
    mean = total / (E * C)
    inv = lax.rsqrt(square / (E * C) - mean * mean + NORM_EPS)
    for b in range(E):
        normed[b] = ((tok_pad[b] - mean) * inv * first_gain[b * C : (b + 1) * C].reshape(1, C)).astype(BF16)

    for load in loads[:4]:
        load.wait()

    mine = normed[e]

    half = wall.shape[1] // 2

    def proj_copy(d, part, source, slot):
        cols = slice(part * half, (part + 1) * half)
        return ep_copy(
            d, proj_send.at[source, 0:SB, cols], proj_recv.at[slot, 0:SB, cols],
            s1.at[part], r1.at[part],
        )

    for part in range(2):

        def project(at, size, base=part * half):
            at = pl.multiple_of(base + at, size)
            total = jnp.dot(mine, wall[:, pl.ds(at, size)], preferred_element_type=F32)
            total = total.reshape(E, PB, size)
            proj_own[:, :, pl.ds(at, size)] = total
            proj_send[:, :, pl.ds(at, size)] = total.astype(BF16)

        tiles(half, project)
        each(1, E, lambda d: proj_copy(d, part, lax.rem(e + d, E), e).start())

    heads = w_input.shape[0]
    pre_i = jnp.zeros((SP, heads), F32)
    pre_f = jnp.zeros((SP, heads), F32)
    across = (((1,), (1,)), ((), ()))
    for b in range(E):
        cols = slice(b * C, (b + 1) * C)
        pre_i = pre_i + lax.dot_general(normed[b], w_input[:, cols], across, preferred_element_type=F32)
        pre_f = pre_f + lax.dot_general(normed[b], w_forget[:, cols], across, preferred_element_type=F32)
    pre_gate[0] = (pre_i + input_bias[...]).reshape(E, PB, heads)
    pre_gate[1] = (pre_f + forget_bias[...]).reshape(E, PB, heads)
    my_i = pre_gate[0, e][:SB]
    my_f = pre_gate[1, e][:SB]
    lane = lax.broadcasted_iota(jnp.int32, my_i.shape, 1)
    diag = lax.broadcasted_iota(jnp.int32, (SB, SB), 0) == lax.broadcasted_iota(jnp.int32, (SB, SB), 1)
    keeps, admits = [], []
    for h in range(Hl):
        i_col = jnp.sum(jnp.where(lane == t * Hl + h, my_i, 0.0), axis=1, keepdims=True)
        f_col = jnp.sum(jnp.where(lane == t * Hl + h, my_f, 0.0), axis=1, keepdims=True)
        log_sig = jnp.minimum(f_col, 0.0) - jnp.log1p(jnp.exp(-jnp.abs(f_col)))
        carried = log_sig + jnp.sum(jnp.where(diag, max_state[h : h + 1, :], 0.0), axis=1, keepdims=True)
        top = jnp.maximum(carried, i_col)
        keep = jnp.exp(carried - top)
        new_max[h : h + 1, :] = jnp.sum(jnp.where(diag, top, 0.0), axis=0, keepdims=True)
        keep_out[:, h : h + 1] = keep
        keeps.append(keep)
        admits.append(jnp.exp(i_col - top))
    mix_rows[...] = jnp.zeros_like(mix_rows)
    loads[4].wait()

    for part in range(2):
        each(1, E, lambda d: proj_copy(d, part, 0, lax.rem(e + E - d, E)).wait_recv())
    summed = proj_own[e]
    for d in range(1, E):
        summed = summed + proj_recv[lax.rem(e + E - d, E)].astype(F32)
    rounded = summed
    gains = head_gain[pl.ds(pl.multiple_of(t * VW, VW), VW)].reshape(1, VW)
    for h in range(Hl):
        q8 = rounded[:, h * DK : (h + 1) * DK] * (DK ** -0.5)
        k = rounded[:SB, QW + h * DK : QW + (h + 1) * DK]
        v = rounded[:SB, 2 * QW + h * DV : 2 * QW + (h + 1) * DV]
        gate_o = rounded[:SB, 2 * QW + VW + h * DV : 2 * QW + VW + (h + 1) * DV]
        turned = q8.T
        for s in range(SB):
            rows_out[s : s + 1, :] = jnp.sum(
                turned[:, s : s + 1] * cell[s, h], axis=0, keepdims=True
            )
        q_k = jnp.sum(q8[:SB] * k, axis=1, keepdims=True)
        read = keeps[h] * rows_out[0:SB, :] + (admits[h] * q_k) * v
        centred = read - jnp.mean(read, axis=1, keepdims=True)
        var = jnp.mean(centred * centred, axis=1, keepdims=True)
        mix_rows[0:SB, h * DV : (h + 1) * DV] = (
            centred * lax.rsqrt(var + HEAD_EPS) * gains[:, h * DV : (h + 1) * DV]
            * jax.nn.sigmoid(gate_o)
        )
        admitted = admits[h] * k
        key_out[:, h, :] = admitted
        value_out[:, h, :] = v
        new_norm[:, h, :] = keeps[h] * norm_state[:, h, :] + admitted
    mix_all[e] = mix_rows[...].astype(BF16)

    each(1, E, lambda d: ep_copy(d, mix_all.at[e, 0:SB], mix_all.at[e, 0:SB], s2, r2).start())
    loads[5].wait()
    each(1, E, lambda d: ep_copy(d, mix_all.at[e, 0:SB], mix_all.at[lax.rem(e + E - d, E), 0:SB], s2, r2).wait_recv())
    mix_mat[...] = mix_all[...].astype(F32).reshape(SP, VW).astype(BF16)

    def out_project(at, size):
        part = jnp.dot(mix_mat[...], wproj[:, pl.ds(at, size)], preferred_element_type=F32)
        term_send[:, :, pl.ds(at, size)] = part.reshape(T, PB, size)

    tiles(C, out_project)
    each(1, T, lambda d: tp_copy(d, term_send.at[lax.rem(t + d, T), 0:SB], term_recv.at[t, 0:SB], s3, r3).start())
    term_recv[t] = term_send[t]
    out_rows[...] = tok_pad[e].reshape(E, PB, C)
    each(1, T, lambda d: tp_copy(d, term_send.at[0, 0:SB], term_recv.at[lax.rem(t + T - d, T), 0:SB], s3, r3).wait_recv())
    mixer = term_recv[0]
    for b in range(1, T):
        mixer = mixer + term_recv[b]
    stream_all[e, t] = (out_rows[t] + mixer).astype(BF16)

    each(1, G, lambda d: all_copy(d, stream_all.at[e, t, 0:SB], stream_all.at[e, t, 0:SB], s4, r4).start())

    def take_stream(d):
        be, bt = behind(d)
        all_copy(d, stream_all.at[e, t, 0:SB], stream_all.at[be, bt, 0:SB], s4, r4).wait_recv()

    for load in loads[6:8]:
        load.wait()
    each(1, G, take_stream)
    total = jnp.zeros((SP, 1), F32)
    square = jnp.zeros((SP, 1), F32)
    for b in range(E):
        x = stream_all[b].astype(F32).reshape(SP, C)
        tok_pad[b] = x
        total = total + jnp.sum(x, axis=1, keepdims=True)
        square = square + jnp.sum(x * x, axis=1, keepdims=True)
    mean = total / (E * C)
    inv = lax.rsqrt(square / (E * C) - mean * mean + NORM_EPS)
    for b in range(E):
        second[:, b * C : (b + 1) * C] = (
            (tok_pad[b] - mean) * inv * second_gain[b * C : (b + 1) * C].reshape(1, C)
        ).astype(BF16)

    def hidden(at, size):
        g = jnp.dot(second[...], gate[:, pl.ds(at, size)], preferred_element_type=F32)
        u = jnp.dot(second[...], up[:, pl.ds(at, size)], preferred_element_type=F32)
        act[:, pl.ds(at, size)] = (g * jax.nn.sigmoid(g) * u).astype(BF16)

    tiles(gate.shape[1], hidden)
    loads[8].wait()

    mid = down.shape[1] // 2

    def exp_copy(d, part, source, slot):
        cols = slice(part * mid, (part + 1) * mid)
        return tp_copy(
            d, exp_send.at[source, 0:SB, cols], exp_recv.at[slot, 0:SB, cols],
            s5.at[part], r5.at[part],
        )

    for part in range(2):

        def lower(at, size, base=part * mid):
            at = pl.multiple_of(base + at, size)
            total = jnp.dot(act[...], down[:, pl.ds(at, size)], preferred_element_type=F32)
            exp_send[:, :, pl.ds(at, size)] = total.reshape(T, PB, size).astype(BF16)

        tiles(mid, lower)
        each(1, T, lambda d: exp_copy(d, part, lax.rem(t + d, T), t).start())
    exp_recv[t] = exp_send[t]
    for part in range(2):
        each(1, T, lambda d: exp_copy(d, part, 0, lax.rem(t + T - d, T)).wait_recv())
    whole = exp_recv[0].astype(F32)
    for b in range(1, T):
        whole = whole + exp_recv[b].astype(F32)
    weighted = whole.astype(BF16).astype(F32) * weight_rows[t][:, 0:1]
    for b in range(E):
        final_send[b] = weighted[:, b * C : (b + 1) * C].astype(BF16)

    def send_final(d):
        pe, pt = peer(d)
        all_copy(d, final_send.at[pe, 0:SB], final_recv.at[e, t, 0:SB], s6, r6).start()

    each(1, G, send_final)
    final_recv[e, t] = final_send[e]

    def take_final(d):
        be, bt = behind(d)
        all_copy(d, final_send.at[0, 0:SB], final_recv.at[be, bt, 0:SB], s6, r6).wait_recv()

    each(1, G, take_final)
    moe = final_recv[0].astype(F32)
    for b in range(1, E):
        moe = moe + final_recv[b].astype(F32)
    done = (tok_pad[e] + moe.reshape(SP, C)).astype(BF16)
    back_row = lax.broadcasted_iota(jnp.int32, (S, SP), 0)
    back_col = lax.broadcasted_iota(jnp.int32, (S, SP), 1)
    gather = jnp.where((back_row // SB) * PB + back_row % SB == back_col, 1.0, 0.0).astype(BF16)
    layer_out[...] = jnp.dot(gather, done, preferred_element_type=F32).astype(BF16)

    each(1, E, lambda d: ep_copy(d, tokens, tok_all.at[e], s0, r0).wait_send())
    for part in range(2):
        each(1, E, lambda d: proj_copy(d, part, 0, e).wait_send())
    each(1, E, lambda d: ep_copy(d, mix_all.at[e, 0:SB], mix_all.at[e, 0:SB], s2, r2).wait_send())
    each(1, T, lambda d: tp_copy(d, term_send.at[0, 0:SB], term_recv.at[t, 0:SB], s3, r3).wait_send())
    each(1, G, lambda d: all_copy(d, stream_all.at[e, t, 0:SB], stream_all.at[e, t, 0:SB], s4, r4).wait_send())
    for part in range(2):
        each(1, T, lambda d: exp_copy(d, part, 0, t).wait_send())
    each(1, G, lambda d: all_copy(d, final_send.at[0, 0:SB], final_recv.at[e, t, 0:SB], s6, r6).wait_send())


def on_device(
    E, T,
    tokens, first_gain, w_query, w_key, w_value, w_outgate, w_input, w_forget,
    input_bias, forget_bias, head_gain, w_project, cell_state, norm_state, max_state,
    second_gain, routes, route_weight, expert_gate, expert_up, expert_down,
):
    S, C = tokens.shape
    SB, Hl, DK, DV = cell_state.shape
    D = first_gain.shape[0]
    FL = expert_gate.shape[2]
    PB = -(-SB // 8) * 8
    SP = E * PB
    heads = w_input.shape[1]
    width = 2 * Hl * (DK + DV)
    VW = Hl * DV
    vmem = pl.BlockSpec(memory_space=pltpu.VMEM)
    hbm = pl.BlockSpec(memory_space=pl.ANY)
    V = pltpu.VMEM
    dma = pltpu.SemaphoreType.DMA
    G = E * T
    layer_out, new_norm, new_max, admitted, values, keep = pl.pallas_call(
        functools.partial(layer_kernel, E, T, SB, PB),
        out_shape=(
            jax.ShapeDtypeStruct((S, C), BF16),
            jax.ShapeDtypeStruct((SB, Hl, DK), F32),
            jax.ShapeDtypeStruct((Hl, SB), F32),
            jax.ShapeDtypeStruct((SB, Hl, DK), F32),
            jax.ShapeDtypeStruct((SB, Hl, DV), F32),
            jax.ShapeDtypeStruct((SB, Hl), F32),
        ),
        in_specs=[vmem] * 12 + [hbm] * 9,
        out_specs=(vmem,) * 6,
        scratch_shapes=[
            V((C, width), BF16),
            V(w_project.shape, BF16),
            V(cell_state.shape, F32),
            V((D, FL), BF16),
            V((D, FL), BF16),
            V((FL, D), BF16),
            V((E, S, C), BF16),
            V((E, SP, C), F32),
            V((E, SP, C), BF16),
            V((2, E, PB, heads), F32),
            V((E, PB, width), F32),
            V((E, PB, width), BF16),
            V((E, PB, width), BF16),
            V((PB, DV), F32),
            V((PB, VW), F32),
            V((E, PB, VW), BF16),
            V((SP, VW), BF16),
            V((T, PB, C), F32),
            V((T, PB, C), F32),
            V((E, T, PB, C), BF16),
            V((SP, D), BF16),
            V((SP, FL), BF16),
            V((T, PB, D), BF16),
            V((T, PB, D), BF16),
            V((E, PB, C), BF16),
            V((E, T, PB, C), BF16),
            V((E, PB, 128), F32),
            V((E, PB, C), F32),
            dma((9,)),
            dma((E,)), dma((E,)), dma((2, E)), dma((2, E)), dma((E,)), dma((E,)),
            dma((T,)), dma((T,)), dma((G,)), dma((G,)), dma((2, T)), dma((2, T)),
            dma((G,)), dma((G,)),
        ],
        compiler_params=pltpu.CompilerParams(
            collective_id=0, has_side_effects=True, vmem_limit_bytes=56 * 1024 * 1024
        ),
        name="layer",
    )(
        tokens, first_gain, w_input.T, w_forget.T,
        input_bias.reshape(1, heads), forget_bias.reshape(1, heads),
        head_gain, norm_state, max_state.T, second_gain,
        routes.T, route_weight.T,
        w_query, w_key, w_value, w_outgate, w_project, cell_state,
        expert_gate, expert_up, expert_down,
    )
    new_cell = (
        keep[:, :, None, None] * cell_state + admitted[:, :, :, None] * values[:, :, None, :]
    )
    return layer_out, new_cell, new_norm, new_max.T


def solution(mesh):
    placed = (
        P("grp", "ep"), P(), P("ep", "tp"), P("ep", "tp"), P("ep", "tp"), P("ep", "tp"),
        P(), P(), P(), P(), P(), P("tp", "ep"),
        P(("grp", "ep"), "tp", None, None), P(("grp", "ep"), "tp", None), P(("grp", "ep"), "tp"),
        P(), P("grp", None), P("grp", None),
        P("ep", None, "tp"), P("ep", None, "tp"), P("ep", "tp", None),
    )
    return jax.shard_map(
        functools.partial(on_device, mesh.shape["ep"], mesh.shape["tp"]),
        mesh=mesh,
        in_specs=placed,
        out_specs=(
            P("grp", "ep"),
            P(("grp", "ep"), "tp", None, None),
            P(("grp", "ep"), "tp", None),
            P(("grp", "ep"), "tp"),
        ),
        check_vma=False,
    )
```
